32 devices in a mesh: sp: 8 (over z, y), tp: 4 (over x, core).
Axes of the slice: x: 2, y: 2, z: 4, core: 2. Of those that a mesh axis runs over, the one named last changes fastest.
Arguments:
- stream: bfloat16 [2048, 2048], P('sp'), may hold values from -6 to 6
- pooled_in: bfloat16 [2048, 1024], P('sp', 'tp'), may hold values from -6 to 6
- pool_weight: bfloat16 [4, 256, 256], P('tp'), may hold values from -0.375 to 0.375
- pool_scale: float32 [1024], P('tp'), may hold values from 0.1 to 1.9
- out_weight: bfloat16 [1024, 2048], replicated, may hold values from -0.1875 to 0.1875
- norm_gain: float32 [2048], replicated, may hold values from 0.1 to 1.9
- routes: int32 [2048, 3], P('sp'), may hold values from 0 to 7, all different within a row; in each aligned block of 64 rows (0 to 63, 64 to 127, ...) at most 48 rows name the same one
- route_weights: float32 [2048, 3], P('sp'), may hold values from 0.25 to 2.5
- expert_gate: bfloat16 [8, 2048, 2048], P('sp', None, 'tp'), may hold values from -0.125 to 0.125
- expert_up: bfloat16 [8, 2048, 2048], P('sp', None, 'tp'), may hold values from -0.125 to 0.125
- expert_down: bfloat16 [8, 2048, 2048], P('sp', 'tp'), may hold values from -0.125 to 0.125
- shared_gate: bfloat16 [2048, 512], P(None, 'tp'), may hold values from -0.125 to 0.125
- shared_up: bfloat16 [2048, 512], P(None, 'tp'), may hold values from -0.125 to 0.125
- shared_down: bfloat16 [512, 2048], P('tp'), may hold values from -0.25 to 0.25
Outputs:
- layer_out: bfloat16 [2048, 2048], P(('sp', 'tp'))
The draws below stay inside these ranges and needn't reach their ends.
Inputs may be any that keep to these rules, and one draw needn't show every extreme that they name: `routes`: each row names 3 different experts. In each aligned block of 64 rows (the rows of one device in the layer's output) no expert is named by more than 48 rows, a bound that some block reaches.
All inputs are finite; a program needn't handle non-finite values.
Results may differ from the reference program's by a relative error of at most 0.012.
Values may be sent and summed in bfloat16 or wider, within the bound.
No kernel may reach another device: no remote copies, remote signals or barrier semaphores. Data moves between devices by JAX's collectives and lax.ppermute only.
A program may use at most 128 MiB of HBM per device.

```python
import math
import jax
import jax.numpy as jnp
import numpy as np
from jax import lax

D = 2048
WINDOWS = 4
PW = 1024
PG = 256
REACH = 16
EFF = 2048
SFF = 512
TOPK = 3
TOKENS = 2048
ROWS_DEV = 64
EXPERTS = 8
CAP = 48
N_SP = 8
N_TP = 4


def shard_levels(own_key, dims, pieces, least, top_value):
    loudness, own = 1.0, jax.random.fold_in(own_key, 6)
    for dim, shards_of in pieces:
        heights = jnp.exp(jax.random.uniform(jax.random.fold_in(own, dim), (shards_of,), jnp.float32, least / len(pieces), top_value / len(pieces)))
        loudness = loudness * jnp.repeat(heights, dims[dim] // shards_of).reshape([-1 if axis == dim else 1 for axis in range(len(dims))])
    return loudness


def assign_block(own_key, own, number, rows, amount, top, most, lean):
    sequence = jax.random.permutation(own_key, amount)
    crowded, usual = shares(amount, rows * top, most, lean, True), shares(amount, rows * top, most, lean, False)
    places = jnp.arange(amount)

    def named(tallies, rotation):
        used = int((tallies > 0).sum())
        fixed = max(1, used // 4)
        moved = fixed + (places - fixed + rotation * (used - fixed)) % max(1, amount - fixed)
        return jnp.zeros((amount,), jnp.int32).at[sequence[jnp.where(places < fixed, places, moved)]].set(jnp.asarray(tallies, jnp.int32))

    tallies = jnp.where(number % 4 == 0, named(crowded, number // 4), named(usual, number - number // 4 - 1))
    mixed = jax.random.permutation(jax.random.fold_in(own, 3), amount)
    source_of, sink = mixed[0:amount // 2 * 2:2], mixed[1:amount // 2 * 2:2]
    slack = jnp.minimum(tallies[source_of] - 1, most - tallies[sink]) // 2
    slack = jnp.where((source_of == sequence[0]) | (sink == sequence[0]) | (tallies[sink] == 0), 0, jnp.maximum(slack, 0))
    moved = jax.random.randint(jax.random.fold_in(own, 4), (amount // 2,), 0, 1 << 20) % (slack + 1)
    tallies = tallies.at[source_of].add(-moved).at[sink].add(moved)
    items = jnp.searchsorted(jnp.cumsum(tallies), jnp.arange(rows * top), side="right").astype(jnp.int32)
    table = items.reshape(top, rows).T
    table = table[jax.random.permutation(jax.random.fold_in(own, 1), rows)]
    rotation = jax.random.randint(jax.random.fold_in(own, 2), (rows, 1), 0, top)
    return jnp.take_along_axis(table, (jnp.arange(top)[None, :] + rotation) % top, axis=1)


def shares(count, total, most, skew, full):
    loads = [(1 << 20) // math.isqrt(rank ** skew) + 1 for rank in range(1, count + 1)]
    largest = most if full else min(most, max(-(-total // count), total * loads[0] // sum(loads)))
    least = 1 if total - largest >= count - 1 else 0
    holding, spare = [largest] + [least] * (count - 1), total - largest - least * (count - 1)
    while spare > 0:
        candidates = [i for i in range(1, count) if holding[i] < largest] or [i for i in range(1, count) if holding[i] < most]
        mass, budget = sum([loads[i] for i in candidates]), spare
        for i in candidates:
            more = min(most - holding[i], max(1, budget * loads[i] // mass), spare)
            holding[i] = holding[i] + more
            spare = spare - more
    return np.array(holding)


def noise(key, dims, scale, bound, pieces=(), held_as=jnp.bfloat16):
    entries = scale * jax.random.normal(key, dims, jnp.float32)
    if pieces:
        entries = entries * shard_levels(key, dims, pieces, -0.22, 0.18)
    return jnp.clip(entries, -bound, bound).astype(held_as)


def setup_inputs(seed: int = 0) -> dict:
    splits = jax.random.split(jax.random.key(seed), 15)
    stream = noise(splits[0], (TOKENS, D), 1.0, 6.0, ((0, 8),))
    pooled_in = noise(splits[1], (TOKENS, PW), 1.0, 6.0, ((0, 8), (1, 4)))
    pool_weight = noise(splits[2], (WINDOWS, PG, PG), PG ** -0.5, 0.375, ((0, 4),))
    pool_scale = jnp.clip(1.0 + 0.18 * jax.random.normal(splits[3], (PW,), jnp.float32), 0.1, 1.9)
    out_weight = noise(splits[4], (PW, D), PW ** -0.5, 0.1875)
    norm_gain = jnp.clip(1.0 + 0.18 * jax.random.normal(splits[5], (D,), jnp.float32), 0.1, 1.9)
    routes_keys = jax.random.split(jax.random.fold_in(splits[6], 1), TOKENS // ROWS_DEV)
    routes_turns = jax.random.permutation(jax.random.fold_in(splits[6], 3), TOKENS // ROWS_DEV)
    routes = jax.vmap(lambda own, number: assign_block(jax.random.fold_in(splits[6], 2), own, number, ROWS_DEV, EXPERTS, TOPK, CAP, 1))(routes_keys, routes_turns).reshape((TOKENS, TOPK))
    route_weights = jnp.clip(jnp.exp(math.log(2.5) - 2.3025851 * jax.random.uniform(splits[7], (TOKENS, TOPK), jnp.float32) ** shard_levels(splits[7], (TOKENS, TOPK), ((0, 8),), -0.2, 0.2)), 0.25, 2.5)
    expert_gate = noise(splits[8], (EXPERTS, D, EFF), D ** -0.5, 0.125, ((0, 8), (2, 4)))
    expert_up = noise(splits[9], (EXPERTS, D, EFF), D ** -0.5, 0.125, ((0, 8), (2, 4)))
    expert_down = noise(splits[10], (EXPERTS, EFF, D), EFF ** -0.5, 0.125, ((0, 8), (1, 4)))
    shared_gate = noise(splits[11], (D, SFF), D ** -0.5, 0.125, ((1, 4),))
    shared_up = noise(splits[12], (D, SFF), D ** -0.5, 0.125, ((1, 4),))
    shared_down = noise(splits[13], (SFF, D), SFF ** -0.5, 0.25, ((0, 4),))
    return {"stream": stream, "pooled_in": pooled_in, "pool_weight": pool_weight, "pool_scale": pool_scale, "out_weight": out_weight, "norm_gain": norm_gain, "routes": routes, "route_weights": route_weights, "expert_gate": expert_gate, "expert_up": expert_up, "expert_down": expert_down, "shared_gate": shared_gate, "shared_up": shared_up, "shared_down": shared_down}


EPSILON = 1e-06

def down_rounded(hidden, weight):
    group_rows = weight.shape[0] // N_TP
    summed = jnp.zeros((hidden.shape[0], weight.shape[1]), jnp.float32)
    for part_index in range(N_TP):
        partial_value = jnp.dot(hidden[:, part_index * group_rows:(part_index + 1) * group_rows], weight[part_index * group_rows:(part_index + 1) * group_rows], preferred_element_type=jnp.float32)
        summed = summed + lax.optimization_barrier(partial_value.astype(jnp.bfloat16)).astype(jnp.float32)
    return summed

def reference(stream, pooled_in, pool_weight, pool_scale, out_weight, norm_gain, routes, route_weights, expert_gate, expert_up, expert_down, shared_gate, shared_up, shared_down):
    tokens_all = stream.shape[0]
    position = jnp.arange(tokens_all, dtype=jnp.int32)
    group_outs = []
    for group_index in range(WINDOWS):
        window = 2 ** (group_index + 1)
        channels = pooled_in[:, group_index * PG:(group_index + 1) * PG].astype(jnp.float32)
        padded = jnp.concatenate([jnp.zeros((REACH - 1, PG), jnp.float32), channels], 0)
        summed = jnp.zeros_like(channels)
        for lag_step in range(window):
            summed = summed + padded[REACH - 1 - lag_step:REACH - 1 - lag_step + tokens_all]
        counted = jnp.minimum(position + 1, window).astype(jnp.float32)
        pooled = (summed / counted[:, None] - channels).astype(jnp.bfloat16)
        mixed_group = jnp.dot(pooled, pool_weight[group_index], preferred_element_type=jnp.float32)
        mixed_group = mixed_group * pool_scale[group_index * PG:(group_index + 1) * PG]
        group_outs.append(mixed_group.astype(jnp.bfloat16))
    grouped = jnp.concatenate(group_outs, 1)
    mixed_all = jnp.dot(grouped, out_weight, preferred_element_type=jnp.float32)
    residual = (stream.astype(jnp.float32) + mixed_all).astype(jnp.bfloat16)
    resid_wide = residual.astype(jnp.float32)
    normed = (resid_wide * lax.rsqrt(lax.optimization_barrier(jnp.mean(resid_wide * resid_wide, axis=-1, keepdims=True)) + EPSILON) * norm_gain).astype(jnp.bfloat16)
    most_rows = N_SP * N_TP * CAP
    slot_iota = jnp.arange(most_rows, dtype=jnp.int32)
    expert_ids = jnp.arange(EXPERTS, dtype=jnp.int32)

    def one_expert(running, inputs):
        w_gate, w_up, w_down, expert_id = inputs
        chosen = routes == expert_id
        member = jnp.any(chosen, axis=1)
        weight = lax.optimization_barrier(jnp.sum(jnp.where(chosen, route_weights, jnp.zeros_like(route_weights)), axis=1))
        picked = jnp.nonzero(member, size=most_rows, fill_value=0)[0].astype(jnp.int32)
        valid_rows = (slot_iota < jnp.sum(member.astype(jnp.int32))).astype(jnp.float32)
        row_data = normed[picked]
        hidden = (jax.nn.silu(jnp.dot(row_data, w_gate, preferred_element_type=jnp.float32)) * jnp.dot(row_data, w_up, preferred_element_type=jnp.float32)).astype(jnp.bfloat16)
        result = lax.optimization_barrier(down_rounded(hidden, w_down).astype(jnp.bfloat16)).astype(jnp.float32)
        scaled = result * (weight[picked] * valid_rows)[:, None]
        return (running.at[picked].add(scaled), None)
    routed, _ = lax.scan(one_expert, jnp.zeros((tokens_all, D), jnp.float32), (expert_gate, expert_up, expert_down, expert_ids))
    shared_hidden = (jax.nn.silu(jnp.dot(normed, shared_gate, preferred_element_type=jnp.float32)) * jnp.dot(normed, shared_up, preferred_element_type=jnp.float32)).astype(jnp.bfloat16)
    shared = down_rounded(shared_hidden, shared_down)
    return (residual.astype(jnp.float32) + routed + shared).astype(jnp.bfloat16)
```

```python
import jax
import jax.numpy as jnp
from jax import lax
from jax.sharding import PartitionSpec as P

REACH = 16


EPSILON = 1e-06

AXES = ("sp", "tp")
CORE_BIT, X_BIT = 1, 2


def passed_along(value, axis, steps):
    count = lax.axis_size(axis)
    initial, last = (max(0, -steps), min(count, count - steps))
    return lax.ppermute(value, axis, [(source, source + steps) for source in range(initial, last)])


def swapped(value, flip):
    count = lax.axis_size(AXES)
    return lax.ppermute(value, AXES, [(source, source ^ flip) for source in range(count)])


def slot_positions(route_block, n_experts, capacity):
    flat_ids = route_block.reshape(-1)
    onehot = (flat_ids[:, None] == jnp.arange(n_experts, dtype=jnp.int32)[None, :]).astype(
        jnp.int32
    )
    earlier = jnp.cumsum(onehot, axis=0) - onehot
    rank_in = jnp.sum(earlier * onehot, axis=1)
    return flat_ids * capacity + rank_in


def mixer(stream, pooled_in, pool_weight, pool_scale, out_weight, norm_gain):
    tok_dev, group_width = pooled_in.shape
    tp_index = lax.axis_index("tp")
    sp_index = lax.axis_index("sp")
    window = lax.shift_left(jnp.int32(2), tp_index)
    rim_rows = passed_along(pooled_in[tok_dev - (REACH - 1) :], "sp", 1)
    padded = jnp.concatenate([rim_rows, pooled_in], 0).astype(jnp.float32)
    summed = jnp.zeros((tok_dev, group_width), jnp.float32)
    for lag_step in range(REACH):
        enabled = (lag_step < window).astype(jnp.float32)
        summed = summed + padded[REACH - 1 - lag_step : REACH - 1 - lag_step + tok_dev] * enabled
    position = sp_index * tok_dev + jnp.arange(tok_dev, dtype=jnp.int32)
    counted = jnp.minimum(position + 1, window).astype(jnp.float32)
    pooled = (summed / counted[:, None] - padded[REACH - 1 :]).astype(jnp.bfloat16)
    group_mix = (
        jnp.dot(pooled, pool_weight[0], preferred_element_type=jnp.float32) * pool_scale
    ).astype(jnp.bfloat16)
    mixed_all = jnp.dot(
        lax.all_gather(group_mix, "tp", axis=1, tiled=True),
        out_weight,
        preferred_element_type=jnp.float32,
    )
    residual = (stream.astype(jnp.float32) + mixed_all).astype(jnp.bfloat16)
    resid_wide = residual.astype(jnp.float32)
    normed = (
        resid_wide
        * lax.rsqrt(jnp.mean(resid_wide * resid_wide, axis=-1, keepdims=True) + EPSILON)
        * norm_gain
    ).astype(jnp.bfloat16)
    return residual, normed


def gated(rows_in, gate, up):
    return (
        jax.nn.silu(jnp.dot(rows_in, gate, preferred_element_type=jnp.float32))
        * jnp.dot(rows_in, up, preferred_element_type=jnp.float32)
    ).astype(jnp.bfloat16)


def routed_plan(
    residual, normed, routes, route_weights, expert_gate, expert_up, expert_down,
    shared_gate, shared_up, shared_down,
):
    tok_dev, model_width = residual.shape
    tp_size = lax.axis_size("tp")
    sp_size = lax.axis_size("sp")
    tp_index = lax.axis_index("tp")
    top_count = routes.shape[1]
    rows_dev = tok_dev // tp_size
    capacity = max(2, 2 * rows_dev * top_count // sp_size)
    own_begin = tp_index * rows_dev
    own_routes = lax.dynamic_slice_in_dim(routes, own_begin, rows_dev, 0)
    own_pos = slot_positions(own_routes, sp_size, capacity)
    own_normed = lax.dynamic_slice_in_dim(normed, own_begin, rows_dev, 0)
    sending = jnp.zeros((sp_size * capacity, model_width), jnp.bfloat16)
    sending = sending.at[own_pos].set(jnp.repeat(own_normed, top_count, axis=0))
    landed = lax.all_to_all(
        sending.reshape(sp_size, capacity, model_width),
        "sp",
        split_axis=0,
        concat_axis=0,
        tiled=True,
    )
    arrived = lax.all_gather(landed[None], "tp", axis=0, tiled=True)
    hidden = gated(arrived.reshape(-1, model_width), expert_gate[0], expert_up[0])
    expert_out = lax.psum_scatter(
        jnp.dot(hidden, expert_down[0], preferred_element_type=jnp.float32).astype(jnp.bfloat16),
        "tp",
        scatter_dimension=0,
        tiled=True,
    )
    returned = lax.all_to_all(
        expert_out.reshape(sp_size, capacity, model_width),
        "sp",
        split_axis=0,
        concat_axis=0,
        tiled=True,
    )
    picked = jnp.take(returned.reshape(-1, model_width), own_pos, axis=0)
    picked = picked.reshape(rows_dev, top_count, model_width)
    own_weights = lax.dynamic_slice_in_dim(route_weights, own_begin, rows_dev, 0)
    routed = jnp.sum(picked.astype(jnp.float32) * own_weights[:, :, None], axis=1)
    hidden = gated(normed, shared_gate, shared_up)
    shared = lax.psum_scatter(
        jnp.dot(hidden, shared_down, preferred_element_type=jnp.float32).astype(jnp.bfloat16),
        "tp",
        scatter_dimension=0,
        tiled=True,
    ).astype(jnp.float32)
    own_resid = lax.dynamic_slice_in_dim(residual, own_begin, rows_dev, 0).astype(jnp.float32)
    return (own_resid + routed + shared).astype(jnp.bfloat16)


def dense_plan(
    residual, normed, routes, route_weights, expert_gate, expert_up, expert_down,
    shared_gate, shared_up, shared_down,
):
    tok_dev, model_width = residual.shape
    tp_size = lax.axis_size("tp")
    sp_size = lax.axis_size("sp")
    tp_index = lax.axis_index("tp")
    sp_index = lax.axis_index("sp")
    rows = tok_dev // tp_size
    y_bit = tp_size
    z_count = sp_size // 2
    half = model_width // 2

    def z_flip(k):
        return 2 * tp_size * k

    gate = jnp.concatenate([expert_gate[0], swapped(expert_gate[0], CORE_BIT)], 1)
    up = jnp.concatenate([expert_up[0], swapped(expert_up[0], CORE_BIT)], 1)
    down = jnp.concatenate([expert_down[0], swapped(expert_down[0], CORE_BIT)], 0)

    experts = jnp.arange(sp_size, dtype=jnp.int32)
    table = jnp.sum(
        jnp.where(routes[None] == experts[:, None, None], route_weights[None], 0.0), axis=2
    )
    mine = lax.all_to_all(table, "sp", split_axis=0, concat_axis=0, tiled=True)
    mine = mine.reshape(z_count, 2, 2, 2, rows)
    core = tp_index % 2
    mine = lax.dynamic_index_in_dim(mine, core, 3, keepdims=False)
    z_index, y_index, x_index = sp_index // 2, sp_index % 2, tp_index // 2
    mine = jnp.take(mine, z_index ^ jnp.arange(z_count), axis=0)
    mine = jnp.where(y_index == 1, mine[:, ::-1], mine)
    mine = jnp.where(x_index == 1, mine[:, :, ::-1], mine)
    scale = jnp.swapaxes(mine, 1, 2)

    own_begin = tp_index * rows
    peer_begin = (tp_index ^ X_BIT) * rows
    own = lax.dynamic_slice_in_dim(normed, own_begin, rows, 0)
    peer = lax.dynamic_slice_in_dim(normed, peer_begin, rows, 0)

    far = {k: swapped(own, z_flip(k)) for k in range(1, z_count)}
    near = swapped(jnp.concatenate([own, peer], 0), y_bit)
    chunks = [jnp.concatenate([own, near[:rows], peer, near[rows:]], 0)]
    order = [2, 3, 1] if z_count == 4 else list(range(1, z_count))
    gathered = {}
    for k in order:
        both = jnp.concatenate([far[k], swapped(far[k], y_bit)], 0)
        gathered[k] = jnp.concatenate([both, swapped(both, X_BIT)], 0)
    chunks += [gathered[k] for k in range(1, z_count)]

    hidden = jnp.stack([gated(chunk, gate, up) for chunk in chunks], 0)
    hidden = hidden.reshape(z_count, 2, 2, rows, -1)

    shared_part = jnp.dot(
        gated(normed, shared_gate, shared_up), shared_down, preferred_element_type=jnp.float32
    ).astype(jnp.bfloat16)
    shared_part = shared_part.reshape(2, 2, rows, model_width)
    kept = lax.dynamic_index_in_dim(shared_part, core, 1, keepdims=False)
    given = lax.dynamic_index_in_dim(shared_part, 1 - core, 1, keepdims=False)
    shared = kept.astype(jnp.float32) + swapped(given, CORE_BIT).astype(jnp.float32)
    shared_own = lax.dynamic_index_in_dim(shared, x_index, 0, keepdims=False)
    shared_peer = lax.dynamic_index_in_dim(shared, 1 - x_index, 0, keepdims=False)

    def project(units, weights, column):
        shape = units.shape[:-1]
        flat = units.reshape(-1, units.shape[-1])
        out = jnp.dot(
            flat, down[:, column : column + half], preferred_element_type=jnp.float32
        )
        return (out * weights.reshape(-1)[:, None]).reshape(*shape, half)

    a_send = project(hidden[:, 1], scale[:, 1], 0)
    a_send = a_send.at[0, 0].add(shared_peer[:, :half])
    a_got = swapped(a_send.astype(jnp.bfloat16), X_BIT)
    b_send = project(hidden[:, :, 1], scale[:, :, 1], half)
    b_got = swapped(b_send.astype(jnp.bfloat16), y_bit)
    a_one = project(hidden[:, 0], scale[:, 0], 0) + a_got.astype(jnp.float32)
    b_one = project(hidden[:, :, 0], scale[:, :, 0], half) + b_got.astype(jnp.float32)
    b_one = b_one.at[0, 1].add(shared_peer[:, half:])
    a_two = swapped(a_one[:, 1].astype(jnp.bfloat16), y_bit)
    b_two = swapped(b_one[:, 1].astype(jnp.bfloat16), X_BIT)
    total = jnp.concatenate(
        [
            a_one[:, 0] + a_two.astype(jnp.float32),
            b_one[:, 0] + b_two.astype(jnp.float32),
        ],
        -1,
    )
    result = total[0] + shared_own
    for k in range(1, z_count):
        result = result + swapped(total[k].astype(jnp.bfloat16), z_flip(k)).astype(jnp.float32)
    own_resid = lax.dynamic_slice_in_dim(residual, own_begin, rows, 0).astype(jnp.float32)
    return (own_resid + result).astype(jnp.bfloat16)


def on_device(
    stream,
    pooled_in,
    pool_weight,
    pool_scale,
    out_weight,
    norm_gain,
    routes,
    route_weights,
    *experts,
):
    residual, normed = mixer(stream, pooled_in, pool_weight, pool_scale, out_weight, norm_gain)
    sp_size = lax.axis_size("sp")
    tp_size = lax.axis_size("tp")
    tok_dev = stream.shape[0]
    capacity = max(2, 2 * (tok_dev // tp_size) * routes.shape[1] // sp_size)
    crowded = 2 * sp_size * tp_size * capacity >= sp_size * tok_dev
    paired = tp_size == 4 and sp_size >= 2 and sp_size & (sp_size - 1) == 0
    plan = dense_plan if crowded and paired else routed_plan
    return plan(residual, normed, routes, route_weights, *experts)


def solution(mesh):
    placed = (
        P("sp", None),
        P("sp", "tp"),
        P("tp", None, None),
        P("tp"),
        P(),
        P(),
        P("sp", None),
        P("sp", None),
        P("sp", None, "tp"),
        P("sp", None, "tp"),
        P("sp", "tp", None),
        P(None, "tp"),
        P(None, "tp"),
        P("tp", None),
    )
    return jax.shard_map(
        on_device, mesh=mesh, in_specs=placed, out_specs=P(("sp", "tp"), None), check_vma=False
    )
```

```python
import functools

import jax
import jax.numpy as jnp
from jax import lax
from jax.experimental import pallas as pl
from jax.experimental.pallas import tpu as pltpu
from jax.sharding import PartitionSpec as P


REACH = 16


EPSILON = 1e-06

AXES = ("sp", "tp")
CORE_BIT, X_BIT = 1, 2
MIB = 2**20


def passed_along(value, axis, steps):
    count = lax.axis_size(axis)
    initial, last = (max(0, -steps), min(count, count - steps))
    return lax.ppermute(value, axis, [(source, source + steps) for source in range(initial, last)])


def swapped(value, flip):
    count = lax.axis_size(AXES)
    return lax.ppermute(value, AXES, [(source, source ^ flip) for source in range(count)])


def slot_positions(route_block, n_experts, capacity):
    flat_ids = route_block.reshape(-1)
    onehot = (flat_ids[:, None] == jnp.arange(n_experts, dtype=jnp.int32)[None, :]).astype(
        jnp.int32
    )
    earlier = jnp.cumsum(onehot, axis=0) - onehot
    rank_in = jnp.sum(earlier * onehot, axis=1)
    return flat_ids * capacity + rank_in


def mixer(stream, pooled_in, pool_weight, pool_scale, out_weight, norm_gain):
    tok_dev, group_width = pooled_in.shape
    tp_index = lax.axis_index("tp")
    sp_index = lax.axis_index("sp")
    window = lax.shift_left(jnp.int32(2), tp_index)
    rim_rows = passed_along(pooled_in[tok_dev - (REACH - 1) :], "sp", 1)
    padded = jnp.concatenate([rim_rows, pooled_in], 0).astype(jnp.float32)
    summed = jnp.zeros((tok_dev, group_width), jnp.float32)
    for lag_step in range(REACH):
        enabled = (lag_step < window).astype(jnp.float32)
        summed = summed + padded[REACH - 1 - lag_step : REACH - 1 - lag_step + tok_dev] * enabled
    position = sp_index * tok_dev + jnp.arange(tok_dev, dtype=jnp.int32)
    counted = jnp.minimum(position + 1, window).astype(jnp.float32)
    pooled = (summed / counted[:, None] - padded[REACH - 1 :]).astype(jnp.bfloat16)
    group_mix = (
        jnp.dot(pooled, pool_weight[0], preferred_element_type=jnp.float32) * pool_scale
    ).astype(jnp.bfloat16)
    mixed_all = jnp.dot(
        lax.all_gather(group_mix, "tp", axis=1, tiled=True),
        out_weight,
        preferred_element_type=jnp.float32,
    )
    residual = (stream.astype(jnp.float32) + mixed_all).astype(jnp.bfloat16)
    resid_wide = residual.astype(jnp.float32)
    normed = (
        resid_wide
        * lax.rsqrt(jnp.mean(resid_wide * resid_wide, axis=-1, keepdims=True) + EPSILON)
        * norm_gain
    ).astype(jnp.bfloat16)
    return residual, normed


def gated(rows_in, gate, up):
    return (
        jax.nn.silu(jnp.dot(rows_in, gate, preferred_element_type=jnp.float32))
        * jnp.dot(rows_in, up, preferred_element_type=jnp.float32)
    ).astype(jnp.bfloat16)


def routed_plan(
    residual, normed, routes, route_weights, expert_gate, expert_up, expert_down,
    shared_gate, shared_up, shared_down,
):
    tok_dev, model_width = residual.shape
    tp_size = lax.axis_size("tp")
    sp_size = lax.axis_size("sp")
    tp_index = lax.axis_index("tp")
    top_count = routes.shape[1]
    rows_dev = tok_dev // tp_size
    capacity = max(2, 2 * rows_dev * top_count // sp_size)
    own_begin = tp_index * rows_dev
    own_routes = lax.dynamic_slice_in_dim(routes, own_begin, rows_dev, 0)
    own_pos = slot_positions(own_routes, sp_size, capacity)
    own_normed = lax.dynamic_slice_in_dim(normed, own_begin, rows_dev, 0)
    sending = jnp.zeros((sp_size * capacity, model_width), jnp.bfloat16)
    sending = sending.at[own_pos].set(jnp.repeat(own_normed, top_count, axis=0))
    landed = lax.all_to_all(
        sending.reshape(sp_size, capacity, model_width),
        "sp",
        split_axis=0,
        concat_axis=0,
        tiled=True,
    )
    arrived = lax.all_gather(landed[None], "tp", axis=0, tiled=True)
    hidden = gated(arrived.reshape(-1, model_width), expert_gate[0], expert_up[0])
    expert_out = lax.psum_scatter(
        jnp.dot(hidden, expert_down[0], preferred_element_type=jnp.float32).astype(jnp.bfloat16),
        "tp",
        scatter_dimension=0,
        tiled=True,
    )
    returned = lax.all_to_all(
        expert_out.reshape(sp_size, capacity, model_width),
        "sp",
        split_axis=0,
        concat_axis=0,
        tiled=True,
    )
    picked = jnp.take(returned.reshape(-1, model_width), own_pos, axis=0)
    picked = picked.reshape(rows_dev, top_count, model_width)
    own_weights = lax.dynamic_slice_in_dim(route_weights, own_begin, rows_dev, 0)
    routed = jnp.sum(picked.astype(jnp.float32) * own_weights[:, :, None], axis=1)
    hidden = gated(normed, shared_gate, shared_up)
    shared = lax.psum_scatter(
        jnp.dot(hidden, shared_down, preferred_element_type=jnp.float32).astype(jnp.bfloat16),
        "tp",
        scatter_dimension=0,
        tiled=True,
    ).astype(jnp.float32)
    own_resid = lax.dynamic_slice_in_dim(residual, own_begin, rows_dev, 0).astype(jnp.float32)
    return (own_resid + routed + shared).astype(jnp.bfloat16)


def pool_kernel(rim_ref, pooled_ref, weight_ref, scale_ref, out_ref):
    tok_dev = pooled_ref.shape[0]
    window = lax.shift_left(jnp.int32(2), lax.axis_index("tp"))
    channels = pooled_ref[...].astype(jnp.float32)
    summed = jnp.concatenate([rim_ref[...].astype(jnp.float32), channels], 0)
    chosen, reach = summed, 1
    while reach < REACH:
        summed = summed + pltpu.roll(summed, reach, 0)
        reach *= 2
        chosen = jnp.where(window == reach, summed, chosen)
    position = lax.axis_index("sp") * tok_dev + lax.broadcasted_iota(jnp.int32, (tok_dev, 1), 0)
    counted = jnp.minimum(position + 1, window).astype(jnp.float32)
    pooled = (chosen[REACH:] / counted - channels).astype(jnp.bfloat16)
    mixed = jnp.dot(pooled, weight_ref[0], preferred_element_type=jnp.float32)
    out_ref[...] = (mixed * scale_ref[...]).astype(jnp.bfloat16)


def norm_kernel(
    grouped_ref, stream_ref, weight_ref, gain_ref, table_ref, packed_ref, resid_ref, wide_ref
):
    rows, width = resid_ref.shape
    tp_index = lax.axis_index("tp")
    own = pl.ds(pl.multiple_of(tp_index * rows, rows), rows)
    peer = pl.ds(pl.multiple_of((tp_index ^ X_BIT) * rows, rows), rows)

    def both(ref, cols=slice(None)):
        return jnp.concatenate([ref[own, cols], ref[peer, cols]], 0)

    grouped = both(grouped_ref)
    squares = jnp.zeros((2 * rows, 1), jnp.float32)
    block = min(512, width)
    for start in range(0, width, block):
        cols = slice(start, start + block)
        mixed = jnp.dot(grouped, weight_ref[:, cols], preferred_element_type=jnp.float32)
        residual = (both(stream_ref, cols).astype(jnp.float32) + mixed).astype(jnp.bfloat16)
        resid_ref[:, cols] = residual[:rows]
        wide = residual.astype(jnp.float32)
        wide_ref[:, cols] = wide
        squares = squares + jnp.sum(wide * wide, axis=1, keepdims=True)
    factor = lax.rsqrt(squares / width + EPSILON)
    for start in range(0, width, block):
        cols = slice(start, start + block)
        packed_ref[:, cols] = (wide_ref[:, cols] * factor * gain_ref[:, cols]).astype(jnp.bfloat16)
    packed_ref[:, width:] = both(table_ref)


def expert_kernel(n_pieces, n_outs, with_shared, *refs):
    pieces = refs[:n_pieces]
    weights = refs[n_pieces : n_pieces + (12 if with_shared else 6)]
    outs = refs[n_pieces + len(weights) :][:n_outs]
    rows_ref, scale_ref, hidden_ref, shared_ref = refs[-4:]
    width = outs[0].shape[1]
    experts = lax.axis_size("sp")
    mine = lax.axis_index("sp")
    begin = 0
    for piece in pieces:
        count = piece.shape[0]
        rows_ref[begin : begin + count] = piece[:, :width]
        marks = piece[:, width:].astype(jnp.float32)
        lane = lax.broadcasted_iota(jnp.int32, marks.shape, 1)
        named = (lane == mine) | (lane == mine + experts)
        scale_ref[begin : begin + count] = jnp.sum(
            jnp.where(named, marks, 0.0), axis=1, keepdims=True
        )
        begin += count

    def fill(target, gates, ups, block):
        column = 0
        for gate, up in zip(gates, ups):
            for start in range(0, gate.shape[1], block):
                cols = slice(start, start + block)
                a = jnp.dot(rows_ref[...], gate[:, cols], preferred_element_type=jnp.float32)
                b = jnp.dot(rows_ref[...], up[:, cols], preferred_element_type=jnp.float32)
                target[:, column : column + block] = (jax.nn.silu(a) * b).astype(jnp.bfloat16)
                column += block

    def product(source, downs, cols):
        total, column = None, 0
        for down in downs:
            depth = down.shape[0]
            part = jnp.dot(
                source[:, column : column + depth], down[:, cols],
                preferred_element_type=jnp.float32,
            )
            total = part if total is None else total + part
            column += depth
        return total

    fill(hidden_ref, weights[0:2], weights[2:4], 256)
    if with_shared:
        fill(shared_ref, weights[6:8], weights[8:10], 128)
    share = begin // n_outs
    block = min(512, width)
    for start in range(0, width, block):
        cols = slice(start, start + block)
        value = product(hidden_ref, weights[4:6], cols) * scale_ref[...]
        if with_shared:
            value = value + product(shared_ref, weights[10:12], cols)
        value = value.astype(jnp.bfloat16)
        for place, out in enumerate(outs):
            out[:, cols] = value[place * share : (place + 1) * share]


def in_vmem(count):
    return [pl.BlockSpec(memory_space=pltpu.VMEM)] * count


def run_expert(pieces, weights, n_outs, width):
    count = sum(piece.shape[0] for piece in pieces)
    with_shared = len(weights) == 12
    hidden = weights[0].shape[1] * 2
    shared = weights[6].shape[1] * 2 if with_shared else 128
    out = jax.ShapeDtypeStruct((count // n_outs, width), jnp.bfloat16)
    return pl.pallas_call(
        functools.partial(expert_kernel, len(pieces), n_outs, with_shared),
        out_shape=[out] * n_outs,
        in_specs=in_vmem(len(pieces) + len(weights)),
        out_specs=in_vmem(n_outs),
        scratch_shapes=[
            pltpu.VMEM((count, width), jnp.bfloat16),
            pltpu.VMEM((count, 1), jnp.float32),
            pltpu.VMEM((count, hidden), jnp.bfloat16),
            pltpu.VMEM((count, shared), jnp.bfloat16),
        ],
        compiler_params=pltpu.CompilerParams(vmem_limit_bytes=16 * MIB),
    )(*pieces, *weights)


def tied(*values):
    return lax.optimization_barrier(values)


def dense_plan(
    stream, pooled_in, pool_weight, pool_scale, out_weight, norm_gain, routes, route_weights,
    expert_gate, expert_up, expert_down, shared_gate, shared_up, shared_down,
):
    tok_dev, width = stream.shape
    tp_size = lax.axis_size("tp")
    sp_size = lax.axis_size("sp")
    rows = tok_dev // tp_size
    f32, bf16 = jnp.float32, jnp.bfloat16
    y_bit = tp_size
    z_bits = [2 * tp_size * k for k in range(sp_size // 2)]

    rim_rows = passed_along(pooled_in[tok_dev - REACH :], "sp", 1)
    weights = []
    for weight in (expert_gate[0], expert_up[0], expert_down[0]):
        weights += [weight, swapped(weight, CORE_BIT)]
    shared_weights = []
    for weight in (shared_gate, shared_up, shared_down):
        shared_weights += [weight, swapped(weight, CORE_BIT)]

    experts = jnp.arange(sp_size, dtype=jnp.int32)
    table = jnp.sum(
        jnp.where(routes[:, :, None] == experts, route_weights[:, :, None], 0.0), axis=1
    )
    high = lax.reduce_precision(table, 8, 7)
    table = jnp.concatenate([high, table - high], 1).astype(bf16)
    lanes = -(-2 * sp_size // 128) * 128
    table = jnp.pad(table, ((0, 0), (0, lanes - 2 * sp_size)))

    group_mix = pl.pallas_call(
        pool_kernel,
        out_shape=jax.ShapeDtypeStruct(pooled_in.shape, bf16),
        in_specs=in_vmem(4),
        out_specs=in_vmem(1)[0],
        compiler_params=pltpu.CompilerParams(vmem_limit_bytes=4 * MIB),
    )(rim_rows, pooled_in, pool_weight, pool_scale[None])
    grouped = lax.all_gather(group_mix, "tp", axis=1, tiled=True)
    pair, own_resid = pl.pallas_call(
        norm_kernel,
        out_shape=[
            jax.ShapeDtypeStruct((2 * rows, width + lanes), bf16),
            jax.ShapeDtypeStruct((rows, width), bf16),
        ],
        in_specs=in_vmem(5),
        out_specs=in_vmem(2),
        scratch_shapes=[pltpu.VMEM((2 * rows, width), f32)],
        compiler_params=pltpu.CompilerParams(vmem_limit_bytes=10 * MIB),
    )(grouped, stream, out_weight, norm_gain[None], table)

    kept, sent, got = {}, {}, {}
    z_1, z_2, _ = z_bits[1:]
    far_2 = swapped(pair[:rows], z_2)
    near = swapped(pair, y_bit)
    next_z = swapped(pair, z_1)
    (kept[0],) = run_expert([pair], weights + shared_weights, 1, width)
    far_2, kept[0] = tied(far_2, kept[0])
    far_3 = swapped(far_2, z_1)
    y_2 = swapped(far_2, y_bit)
    x_2 = swapped(far_2, X_BIT)
    near, far_2 = tied(near, far_2)
    (sent[0],) = run_expert([near], weights, 1, width)
    far_3, sent[0] = tied(far_3, sent[0])
    y_3 = swapped(far_3, y_bit)
    x_3 = swapped(far_3, X_BIT)
    y_2, far_3 = tied(y_2, far_3)
    xy_2 = swapped(y_2, X_BIT)
    next_z, y_2 = tied(next_z, y_2)
    y_1 = swapped(next_z, y_bit)
    sent[0], next_z = tied(sent[0], next_z)
    got[0] = swapped(sent[0], y_bit)
    y_3, next_z = tied(y_3, next_z)
    xy_3 = swapped(y_3, X_BIT)
    xy_2, y_3 = tied(xy_2, y_3)
    kept[2], sent[2] = run_expert([far_2, y_2, x_2, xy_2], weights, 2, width)
    got[2] = swapped(sent[2], X_BIT)
    xy_3, sent[2] = tied(xy_3, sent[2])
    kept[3], sent[3] = run_expert([far_3, y_3, x_3, xy_3], weights, 2, width)
    got[3] = swapped(sent[3], X_BIT)
    y_1, sent[3] = tied(y_1, sent[3])
    kept[1], sent[1] = run_expert([next_z, y_1], weights, 2, width)
    got[1] = swapped(sent[1], y_bit)

    def half(k, which):
        part = slice(which * rows, (which + 1) * rows)
        return kept[k][part].astype(f32) + got[k][part].astype(f32)

    more, flows = {}, {}
    for k in (2, 0, 3, 1):
        flip = X_BIT if k < 2 else y_bit
        more[k] = swapped(half(k, 1).astype(bf16), flip)
    for k in (2, 3, 1):
        flow = (half(k, 0) + more[k].astype(f32)).astype(bf16)
        flows[k] = swapped(flow, z_bits[k])
    result = half(0, 0) + more[0].astype(f32) + own_resid.astype(f32)
    for k in (2, 3, 1):
        result = result + flows[k].astype(f32)
    return result.astype(bf16)


def on_device(
    stream,
    pooled_in,
    pool_weight,
    pool_scale,
    out_weight,
    norm_gain,
    routes,
    route_weights,
    *experts,
):
    sp_size = lax.axis_size("sp")
    tp_size = lax.axis_size("tp")
    tok_dev = stream.shape[0]
    capacity = max(2, 2 * (tok_dev // tp_size) * routes.shape[1] // sp_size)
    crowded = 2 * sp_size * tp_size * capacity >= sp_size * tok_dev
    paired = tp_size == 4 and sp_size == 8
    pooling = (stream, pooled_in, pool_weight, pool_scale, out_weight, norm_gain)
    if crowded and paired:
        return dense_plan(*pooling, routes, route_weights, *experts)
    residual, normed = mixer(*pooling)
    return routed_plan(residual, normed, routes, route_weights, *experts)


def solution(mesh):
    placed = (
        P("sp", None),
        P("sp", "tp"),
        P("tp", None, None),
        P("tp"),
        P(),
        P(),
        P("sp", None),
        P("sp", None),
        P("sp", None, "tp"),
        P("sp", None, "tp"),
        P("sp", "tp", None),
        P(None, "tp"),
        P(None, "tp"),
        P("tp", None),
    )
    return jax.shard_map(
        on_device, mesh=mesh, in_specs=placed, out_specs=P(("sp", "tp"), None), check_vma=False
    )
```

```python
import functools

import jax
import jax.numpy as jnp
from jax import lax
from jax.experimental import pallas as pl
from jax.experimental.pallas import tpu as pltpu
from jax.sharding import PartitionSpec as P


REACH = 16


EPSILON = 1e-06

AXES = ("sp", "tp")
CORE_BIT, X_BIT = 1, 2
MIB = 2**20


def passed_along(value, axis, steps):
    count = lax.axis_size(axis)
    initial, last = (max(0, -steps), min(count, count - steps))
    return lax.ppermute(value, axis, [(source, source + steps) for source in range(initial, last)])


def swapped(value, flip):
    count = lax.axis_size(AXES)
    return lax.ppermute(value, AXES, [(source, source ^ flip) for source in range(count)])


def slot_positions(route_block, n_experts, capacity):
    flat_ids = route_block.reshape(-1)
    onehot = (flat_ids[:, None] == jnp.arange(n_experts, dtype=jnp.int32)[None, :]).astype(
        jnp.int32
    )
    earlier = jnp.cumsum(onehot, axis=0) - onehot
    rank_in = jnp.sum(earlier * onehot, axis=1)
    return flat_ids * capacity + rank_in


def mixer(stream, pooled_in, pool_weight, pool_scale, out_weight, norm_gain):
    tok_dev, group_width = pooled_in.shape
    tp_index = lax.axis_index("tp")
    sp_index = lax.axis_index("sp")
    window = lax.shift_left(jnp.int32(2), tp_index)
    rim_rows = passed_along(pooled_in[tok_dev - (REACH - 1) :], "sp", 1)
    padded = jnp.concatenate([rim_rows, pooled_in], 0).astype(jnp.float32)
    summed = jnp.zeros((tok_dev, group_width), jnp.float32)
    for lag_step in range(REACH):
        enabled = (lag_step < window).astype(jnp.float32)
        summed = summed + padded[REACH - 1 - lag_step : REACH - 1 - lag_step + tok_dev] * enabled
    position = sp_index * tok_dev + jnp.arange(tok_dev, dtype=jnp.int32)
    counted = jnp.minimum(position + 1, window).astype(jnp.float32)
    pooled = (summed / counted[:, None] - padded[REACH - 1 :]).astype(jnp.bfloat16)
    group_mix = (
        jnp.dot(pooled, pool_weight[0], preferred_element_type=jnp.float32) * pool_scale
    ).astype(jnp.bfloat16)
    mixed_all = jnp.dot(
        lax.all_gather(group_mix, "tp", axis=1, tiled=True),
        out_weight,
        preferred_element_type=jnp.float32,
    )
    residual = (stream.astype(jnp.float32) + mixed_all).astype(jnp.bfloat16)
    resid_wide = residual.astype(jnp.float32)
    normed = (
        resid_wide
        * lax.rsqrt(jnp.mean(resid_wide * resid_wide, axis=-1, keepdims=True) + EPSILON)
        * norm_gain
    ).astype(jnp.bfloat16)
    return residual, normed


def gated(rows_in, gate, up):
    return (
        jax.nn.silu(jnp.dot(rows_in, gate, preferred_element_type=jnp.float32))
        * jnp.dot(rows_in, up, preferred_element_type=jnp.float32)
    ).astype(jnp.bfloat16)


def routed_plan(
    residual, normed, routes, route_weights, expert_gate, expert_up, expert_down,
    shared_gate, shared_up, shared_down,
):
    tok_dev, model_width = residual.shape
    tp_size = lax.axis_size("tp")
    sp_size = lax.axis_size("sp")
    tp_index = lax.axis_index("tp")
    top_count = routes.shape[1]
    rows_dev = tok_dev // tp_size
    capacity = max(2, 2 * rows_dev * top_count // sp_size)
    own_begin = tp_index * rows_dev
    own_routes = lax.dynamic_slice_in_dim(routes, own_begin, rows_dev, 0)
    own_pos = slot_positions(own_routes, sp_size, capacity)
    own_normed = lax.dynamic_slice_in_dim(normed, own_begin, rows_dev, 0)
    sending = jnp.zeros((sp_size * capacity, model_width), jnp.bfloat16)
    sending = sending.at[own_pos].set(jnp.repeat(own_normed, top_count, axis=0))
    landed = lax.all_to_all(
        sending.reshape(sp_size, capacity, model_width),
        "sp",
        split_axis=0,
        concat_axis=0,
        tiled=True,
    )
    arrived = lax.all_gather(landed[None], "tp", axis=0, tiled=True)
    hidden = gated(arrived.reshape(-1, model_width), expert_gate[0], expert_up[0])
    expert_out = lax.psum_scatter(
        jnp.dot(hidden, expert_down[0], preferred_element_type=jnp.float32).astype(jnp.bfloat16),
        "tp",
        scatter_dimension=0,
        tiled=True,
    )
    returned = lax.all_to_all(
        expert_out.reshape(sp_size, capacity, model_width),
        "sp",
        split_axis=0,
        concat_axis=0,
        tiled=True,
    )
    picked = jnp.take(returned.reshape(-1, model_width), own_pos, axis=0)
    picked = picked.reshape(rows_dev, top_count, model_width)
    own_weights = lax.dynamic_slice_in_dim(route_weights, own_begin, rows_dev, 0)
    routed = jnp.sum(picked.astype(jnp.float32) * own_weights[:, :, None], axis=1)
    hidden = gated(normed, shared_gate, shared_up)
    shared = lax.psum_scatter(
        jnp.dot(hidden, shared_down, preferred_element_type=jnp.float32).astype(jnp.bfloat16),
        "tp",
        scatter_dimension=0,
        tiled=True,
    ).astype(jnp.float32)
    own_resid = lax.dynamic_slice_in_dim(residual, own_begin, rows_dev, 0).astype(jnp.float32)
    return (own_resid + routed + shared).astype(jnp.bfloat16)


def brought(pairs, sems):
    copies = [
        pltpu.make_async_copy(source, target, sems.at[place])
        for place, (source, target) in enumerate(pairs)
    ]
    for copy in copies:
        copy.start()
    return copies


def pool_kernel(
    rim_ref, pooled_hbm, weight_hbm, scale_hbm, *refs
):
    pieces, (mixed_ref, pooled_ref, weight_ref, scale_ref, sems) = refs[:-5], refs[-5:]
    rows = pieces[0].shape[0] // 2
    tp_index = lax.axis_index("tp")
    copies = brought(
        ((pooled_hbm, pooled_ref), (weight_hbm, weight_ref), (scale_hbm, scale_ref)), sems
    )
    for copy in copies:
        copy.wait()
    tok_dev = pooled_ref.shape[0]
    window = lax.shift_left(jnp.int32(2), lax.axis_index("tp"))
    channels = pooled_ref[...].astype(jnp.float32)
    summed = jnp.concatenate([rim_ref[...].astype(jnp.float32), channels], 0)
    chosen, reach = summed, 1
    while reach < REACH:
        summed = summed + pltpu.roll(summed, reach, 0)
        reach *= 2
        chosen = jnp.where(window == reach, summed, chosen)
    position = lax.axis_index("sp") * tok_dev + lax.broadcasted_iota(jnp.int32, (tok_dev, 1), 0)
    counted = jnp.minimum(position + 1, window).astype(jnp.float32)
    pooled = (chosen[REACH:] / counted - channels).astype(jnp.bfloat16)
    mixed = jnp.dot(pooled, weight_ref[0], preferred_element_type=jnp.float32)
    mixed_ref[...] = (mixed * scale_ref[...]).astype(jnp.bfloat16)
    for flip, piece in enumerate(pieces):
        for place, block in enumerate((tp_index ^ flip, tp_index ^ flip ^ X_BIT)):
            begin = pl.multiple_of(block * rows, rows)
            piece[place * rows : (place + 1) * rows] = mixed_ref[pl.ds(begin, rows)]


def norm_kernel(*refs):
    groups, refs = refs[:-15], refs[-15:]
    routes_hbm, route_weights_hbm, stream_hbm, weight_hbm, gain_hbm = refs[:5]
    packed_ref, resid_ref, wide_ref, stream_ref, weight_ref, gain_ref, table_ref = refs[5:12]
    routes_ref, route_weights_ref, sems = refs[12:]
    rows, width = resid_ref.shape
    parts, depth, _ = weight_ref.shape
    tp_index = lax.axis_index("tp")
    places = [pl.multiple_of(block * rows, rows) for block in (tp_index, tp_index ^ X_BIT)]
    pairs = []
    for part in range(parts):
        begin = pl.multiple_of((tp_index ^ part) * depth, depth)
        pairs.append((weight_hbm.at[pl.ds(begin, depth)], weight_ref.at[part]))
    for place, begin in enumerate(places):
        pairs.append((stream_hbm.at[pl.ds(begin, rows)], stream_ref.at[pl.ds(place * rows, rows)]))
    pairs.append((gain_hbm, gain_ref))
    pairs = [(routes_hbm, routes_ref), (route_weights_hbm, route_weights_ref)] + pairs
    first, second, *copies = brought(pairs, sems)
    first.wait()
    second.wait()

    experts = lax.axis_size("sp")
    named = routes_ref[...]
    share = route_weights_ref[...]
    shape = (table_ref.shape[1], named.shape[1])
    line = lax.broadcasted_iota(jnp.int32, shape, 0)
    table = jnp.zeros(shape, jnp.float32)
    for choice in range(named.shape[0]):
        asked = named[choice : choice + 1]
        hit = (line == asked) | (line == asked + experts)
        table = table + jnp.where(hit, share[choice : choice + 1], 0.0)
    high = table.astype(jnp.bfloat16).astype(jnp.float32)
    table = jnp.where(line < experts, high, table - high)
    table_ref[...] = jnp.transpose(table).astype(jnp.bfloat16)
    for place, begin in enumerate(places):
        packed_ref[place * rows : (place + 1) * rows, width:] = table_ref[pl.ds(begin, rows)]

    block = min(512, width)
    blocks = [slice(start, start + block) for start in range(0, width, block)]
    for part, group in enumerate(groups):
        copies[part].wait()
        for cols in blocks:
            mixed = jnp.dot(
                group[...], weight_ref[part, :, cols], preferred_element_type=jnp.float32
            )
            wide_ref[:, cols] = mixed if part == 0 else wide_ref[:, cols] + mixed
    for copy in copies[parts:]:
        copy.wait()
    squares = jnp.zeros((2 * rows, 1), jnp.float32)
    for cols in blocks:
        residual = (stream_ref[:, cols].astype(jnp.float32) + wide_ref[:, cols]).astype(
            jnp.bfloat16
        )
        resid_ref[:, cols] = residual[:rows]
        wide = residual.astype(jnp.float32)
        wide_ref[:, cols] = wide
        squares = squares + jnp.sum(wide * wide, axis=1, keepdims=True)
    factor = lax.rsqrt(squares / width + EPSILON)
    for cols in blocks:
        packed_ref[:, cols] = (wide_ref[:, cols] * factor * gain_ref[:, cols]).astype(jnp.bfloat16)


def expert_kernel(n_pieces, takes, n_outs, with_shared, *refs):
    pieces = refs[:n_pieces]
    weights = refs[n_pieces : n_pieces + (12 if with_shared else 6)]
    outs = refs[n_pieces + len(weights) :][:n_outs]
    rows_ref, scale_ref, hidden_ref, shared_ref = refs[-4:]
    width = outs[0].shape[1]
    experts = lax.axis_size("sp")
    mine = lax.axis_index("sp")
    begin = 0
    for place, first, count in takes:
        taken = slice(first, first + count)
        rows_ref[begin : begin + count] = pieces[place][taken, :width]
        marks = pieces[place][taken, width:].astype(jnp.float32)
        lane = lax.broadcasted_iota(jnp.int32, marks.shape, 1)
        named = (lane == mine) | (lane == mine + experts)
        scale_ref[begin : begin + count] = jnp.sum(
            jnp.where(named, marks, 0.0), axis=1, keepdims=True
        )
        begin += count

    def fill(target, gates, ups, block):
        column = 0
        for gate, up in zip(gates, ups):
            for start in range(0, gate.shape[1], block):
                cols = slice(start, start + block)
                a = jnp.dot(rows_ref[...], gate[:, cols], preferred_element_type=jnp.float32)
                b = jnp.dot(rows_ref[...], up[:, cols], preferred_element_type=jnp.float32)
                target[:, column : column + block] = (jax.nn.silu(a) * b).astype(jnp.bfloat16)
                column += block

    def product(source, downs, cols):
        total, column = None, 0
        for down in downs:
            depth = down.shape[0]
            part = jnp.dot(
                source[:, column : column + depth], down[:, cols],
                preferred_element_type=jnp.float32,
            )
            total = part if total is None else total + part
            column += depth
        return total

    fill(hidden_ref, weights[0:2], weights[2:4], 256)
    if with_shared:
        fill(shared_ref, weights[6:8], weights[8:10], 128)
    share = begin // n_outs
    block = min(512, width)
    for start in range(0, width, block):
        cols = slice(start, start + block)
        value = product(hidden_ref, weights[4:6], cols) * scale_ref[...]
        if with_shared:
            value = value + product(shared_ref, weights[10:12], cols)
        value = value.astype(jnp.bfloat16)
        for place, out in enumerate(outs):
            out[:, cols] = value[place * share : (place + 1) * share]


def pass_kernel(source, target):
    target[...] = source[...]


def passing(token):
    return pl.pallas_call(
        pass_kernel,
        out_shape=jax.ShapeDtypeStruct(token.shape, token.dtype),
        in_specs=in_vmem(1),
        out_specs=in_vmem(1)[0],
        compiler_params=pltpu.CompilerParams(vmem_limit_bytes=MIB),
    )(token)


def in_vmem(count):
    return [pl.BlockSpec(memory_space=pltpu.VMEM)] * count


def kept_in_hbm(*arrays):
    return [pltpu.with_memory_space_constraint(array, pltpu.HBM) for array in arrays]


def in_hbm(count):
    return [pl.BlockSpec(memory_space=pltpu.HBM)] * count


def run_expert(pieces, weights, n_outs, width, takes=None):
    takes = takes or [(place, 0, piece.shape[0]) for place, piece in enumerate(pieces)]
    count = sum(take[2] for take in takes)
    with_shared = len(weights) == 12
    hidden = weights[0].shape[1] * 2
    shared = weights[6].shape[1] * 2 if with_shared else 128
    out = jax.ShapeDtypeStruct((count // n_outs, width), jnp.bfloat16)
    return pl.pallas_call(
        functools.partial(expert_kernel, len(pieces), tuple(takes), n_outs, with_shared),
        out_shape=[out] * n_outs,
        in_specs=in_vmem(len(pieces) + len(weights)),
        out_specs=in_vmem(n_outs),
        scratch_shapes=[
            pltpu.VMEM((count, width), jnp.bfloat16),
            pltpu.VMEM((count, 1), jnp.float32),
            pltpu.VMEM((count, hidden), jnp.bfloat16),
            pltpu.VMEM((count, shared), jnp.bfloat16),
        ],
        compiler_params=pltpu.CompilerParams(vmem_limit_bytes=16 * MIB),
    )(*pieces, *weights)


def tied(*values):
    return lax.optimization_barrier(values)


def dense_plan(
    stream, pooled_in, pool_weight, pool_scale, out_weight, norm_gain, routes, route_weights,
    expert_gate, expert_up, expert_down, shared_gate, shared_up, shared_down,
):
    tok_dev, width = stream.shape
    tp_size = lax.axis_size("tp")
    sp_size = lax.axis_size("sp")
    rows = tok_dev // tp_size
    f32, bf16 = jnp.float32, jnp.bfloat16
    y_bit = tp_size
    z_bits = [2 * tp_size * k for k in range(sp_size // 2)]

    rim_rows = passed_along(pooled_in[tok_dev - REACH :], "sp", 1)
    weights = []
    for weight in (expert_gate[0], expert_up[0], expert_down[0]):
        weights += [weight, swapped(weight, CORE_BIT)]
    shared_weights = []
    for weight in (shared_gate, shared_up, shared_down):
        shared_weights += [weight, swapped(weight, CORE_BIT)]

    lanes = -(-2 * sp_size // 128) * 128
    piece = jax.ShapeDtypeStruct((2 * rows, pooled_in.shape[1]), bf16)
    pool = pl.pallas_call(
        pool_kernel,
        out_shape=[piece] * tp_size,
        in_specs=in_vmem(1) + in_hbm(3),
        out_specs=in_vmem(tp_size),
        scratch_shapes=[
            pltpu.VMEM(pooled_in.shape, bf16),
            pltpu.VMEM(pooled_in.shape, bf16),
            pltpu.VMEM(pool_weight.shape, bf16),
            pltpu.VMEM((1, pool_scale.size), f32),
            pltpu.SemaphoreType.DMA((3,)),
        ],
        compiler_params=pltpu.CompilerParams(vmem_limit_bytes=4 * MIB),
    )
    rim_rows, weights[1], weights[3] = tied(rim_rows, weights[1], weights[3])
    groups = pool(rim_rows, *kept_in_hbm(pooled_in, pool_weight, pool_scale[None]))
    groups = [swapped(group, flip) if flip else group for flip, group in enumerate(groups)]
    depth = out_weight.shape[0] // tp_size
    pair, own_resid = pl.pallas_call(
        norm_kernel,
        out_shape=[
            jax.ShapeDtypeStruct((2 * rows, width + lanes), bf16),
            jax.ShapeDtypeStruct((rows, width), bf16),
        ],
        in_specs=in_vmem(tp_size) + in_hbm(5),
        out_specs=in_vmem(2),
        scratch_shapes=[
            pltpu.VMEM((2 * rows, width), f32),
            pltpu.VMEM((2 * rows, width), bf16),
            pltpu.VMEM((tp_size, depth, width), bf16),
            pltpu.VMEM((1, width), f32),
            pltpu.VMEM((tok_dev, lanes), bf16),
            pltpu.VMEM(routes.shape[::-1], jnp.int32),
            pltpu.VMEM(routes.shape[::-1], f32),
            pltpu.SemaphoreType.DMA((tp_size + 5,)),
        ],
        compiler_params=pltpu.CompilerParams(vmem_limit_bytes=10 * MIB),
    )(
        *groups,
        *kept_in_hbm(routes.T, route_weights.T, stream, out_weight, norm_gain[None]),
    )

    kept, sent, got = {}, {}, {}
    z_1, z_2, _ = z_bits[1:]
    far_2 = swapped(pair[:rows], z_2)
    near = swapped(pair, y_bit)
    (kept[0],) = run_expert([pair], weights + shared_weights, 1, width)
    far_2, kept[0] = tied(far_2, kept[0])
    far_3 = swapped(far_2, z_1)
    y_2 = swapped(far_2, y_bit)
    x_2 = swapped(far_2, X_BIT)
    near, far_2 = tied(near, far_2)
    pair, far_2 = tied(pair, far_2)
    next_z = swapped(pair, z_1)
    other_z = swapped(near, z_1)
    (sent[0],) = run_expert([near], weights, 1, width)
    y_2, sent[0] = tied(y_2, sent[0])
    xy_2 = swapped(y_2, X_BIT)
    far_3, y_2 = tied(far_3, y_2)
    y_3 = swapped(far_3, y_bit)
    x_3 = swapped(far_3, X_BIT)
    token = passing(jnp.zeros((8, 128), f32))
    y_3, far_3 = tied(y_3, far_3)
    xy_3 = swapped(y_3, X_BIT)
    sent[0], y_3 = tied(sent[0], y_3)
    got[0] = swapped(sent[0], y_bit)
    xy_2, y_3 = tied(xy_2, y_3)
    blocks = [(place, 0, rows) for place in range(4)]
    kept[2], sent[2] = run_expert([far_2, y_2, x_2, xy_2, token], weights, 2, width, blocks)
    got[2] = swapped(sent[2], X_BIT)
    token = passing(token)
    xy_3, sent[2] = tied(xy_3, sent[2])
    kept[3], sent[3] = run_expert([far_3, x_3, y_3, xy_3, token], weights, 2, width, blocks)
    got[3] = swapped(sent[3], y_bit)
    next_z, sent[3] = tied(next_z, sent[3])
    takes = [(0, 0, rows), (1, 0, rows), (0, rows, rows), (1, rows, rows)]
    kept[1], sent[1] = run_expert([next_z, other_z], weights, 2, width, takes)
    got[1] = swapped(sent[1], X_BIT)

    def half(k, which):
        part = slice(which * rows, (which + 1) * rows)
        return kept[k][part].astype(f32) + got[k][part].astype(f32)

    def passed_on(k):
        flip = y_bit if k in (1, 2) else X_BIT
        return swapped(half(k, 1).astype(bf16), flip)

    def finished(k):
        flow = (half(k, 0) + more[k].astype(f32)).astype(bf16)
        return swapped(flow, z_bits[k])

    more, flows = {}, {}
    got[2], sent[1] = tied(got[2], sent[1])
    more[2] = passed_on(2)
    more[0] = passed_on(0)
    got[3], got[2] = tied(got[3], got[2])
    more[3] = passed_on(3)
    more[2], got[3] = tied(more[2], got[3])
    flows[2] = finished(2)
    wide = passing(own_resid.astype(f32))
    base = passing(half(0, 0) + wide)
    more[1] = passed_on(1)
    flows[3] = finished(3)
    flows[1] = finished(1)
    result = base + more[0].astype(f32)
    for k in (2, 3, 1):
        result = result + flows[k].astype(f32)
    return result.astype(bf16)


def on_device(
    stream,
    pooled_in,
    pool_weight,
    pool_scale,
    out_weight,
    norm_gain,
    routes,
    route_weights,
    *experts,
):
    sp_size = lax.axis_size("sp")
    tp_size = lax.axis_size("tp")
    tok_dev = stream.shape[0]
    capacity = max(2, 2 * (tok_dev // tp_size) * routes.shape[1] // sp_size)
    crowded = 2 * sp_size * tp_size * capacity >= sp_size * tok_dev
    paired = tp_size == 4 and sp_size == 8
    pooling = (stream, pooled_in, pool_weight, pool_scale, out_weight, norm_gain)
    if crowded and paired:
        return dense_plan(*pooling, routes, route_weights, *experts)
    residual, normed = mixer(*pooling)
    return routed_plan(residual, normed, routes, route_weights, *experts)


def solution(mesh):
    placed = (
        P("sp", None),
        P("sp", "tp"),
        P("tp", None, None),
        P("tp"),
        P(),
        P(),
        P("sp", None),
        P("sp", None),
        P("sp", None, "tp"),
        P("sp", None, "tp"),
        P("sp", "tp", None),
        P(None, "tp"),
        P(None, "tp"),
        P("tp", None),
    )
    return jax.shard_map(
        on_device, mesh=mesh, in_specs=placed, out_specs=P(("sp", "tp"), None), check_vma=False
    )
```

```python
import functools

import jax
import jax.numpy as jnp
from jax import lax
from jax.experimental import pallas as pl
from jax.experimental.pallas import tpu as pltpu
from jax.sharding import PartitionSpec as P


REACH = 16


EPSILON = 1e-06

AXES = ("sp", "tp")
CORE_BIT, X_BIT = 1, 2
MIB = 2**20


def passed_along(value, axis, steps):
    count = lax.axis_size(axis)
    initial, last = (max(0, -steps), min(count, count - steps))
    return lax.ppermute(value, axis, [(source, source + steps) for source in range(initial, last)])


def swapped(value, flip):
    count = lax.axis_size(AXES)
    return lax.ppermute(value, AXES, [(source, source ^ flip) for source in range(count)])


def slot_positions(route_block, n_experts, capacity):
    flat_ids = route_block.reshape(-1)
    onehot = (flat_ids[:, None] == jnp.arange(n_experts, dtype=jnp.int32)[None, :]).astype(
        jnp.int32
    )
    earlier = jnp.cumsum(onehot, axis=0) - onehot
    rank_in = jnp.sum(earlier * onehot, axis=1)
    return flat_ids * capacity + rank_in


def mixer(stream, pooled_in, pool_weight, pool_scale, out_weight, norm_gain):
    tok_dev, group_width = pooled_in.shape
    tp_index = lax.axis_index("tp")
    sp_index = lax.axis_index("sp")
    window = lax.shift_left(jnp.int32(2), tp_index)
    rim_rows = passed_along(pooled_in[tok_dev - (REACH - 1) :], "sp", 1)
    padded = jnp.concatenate([rim_rows, pooled_in], 0).astype(jnp.float32)
    summed = jnp.zeros((tok_dev, group_width), jnp.float32)
    for lag_step in range(REACH):
        enabled = (lag_step < window).astype(jnp.float32)
        summed = summed + padded[REACH - 1 - lag_step : REACH - 1 - lag_step + tok_dev] * enabled
    position = sp_index * tok_dev + jnp.arange(tok_dev, dtype=jnp.int32)
    counted = jnp.minimum(position + 1, window).astype(jnp.float32)
    pooled = (summed / counted[:, None] - padded[REACH - 1 :]).astype(jnp.bfloat16)
    group_mix = (
        jnp.dot(pooled, pool_weight[0], preferred_element_type=jnp.float32) * pool_scale
    ).astype(jnp.bfloat16)
    mixed_all = jnp.dot(
        lax.all_gather(group_mix, "tp", axis=1, tiled=True),
        out_weight,
        preferred_element_type=jnp.float32,
    )
    residual = (stream.astype(jnp.float32) + mixed_all).astype(jnp.bfloat16)
    resid_wide = residual.astype(jnp.float32)
    normed = (
        resid_wide
        * lax.rsqrt(jnp.mean(resid_wide * resid_wide, axis=-1, keepdims=True) + EPSILON)
        * norm_gain
    ).astype(jnp.bfloat16)
    return residual, normed


def gated(rows_in, gate, up):
    return (
        jax.nn.silu(jnp.dot(rows_in, gate, preferred_element_type=jnp.float32))
        * jnp.dot(rows_in, up, preferred_element_type=jnp.float32)
    ).astype(jnp.bfloat16)


def routed_plan(
    residual, normed, routes, route_weights, expert_gate, expert_up, expert_down,
    shared_gate, shared_up, shared_down,
):
    tok_dev, model_width = residual.shape
    tp_size = lax.axis_size("tp")
    sp_size = lax.axis_size("sp")
    tp_index = lax.axis_index("tp")
    top_count = routes.shape[1]
    rows_dev = tok_dev // tp_size
    capacity = max(2, 2 * rows_dev * top_count // sp_size)
    own_begin = tp_index * rows_dev
    own_routes = lax.dynamic_slice_in_dim(routes, own_begin, rows_dev, 0)
    own_pos = slot_positions(own_routes, sp_size, capacity)
    own_normed = lax.dynamic_slice_in_dim(normed, own_begin, rows_dev, 0)
    sending = jnp.zeros((sp_size * capacity, model_width), jnp.bfloat16)
    sending = sending.at[own_pos].set(jnp.repeat(own_normed, top_count, axis=0))
    landed = lax.all_to_all(
        sending.reshape(sp_size, capacity, model_width),
        "sp",
        split_axis=0,
        concat_axis=0,
        tiled=True,
    )
    arrived = lax.all_gather(landed[None], "tp", axis=0, tiled=True)
    hidden = gated(arrived.reshape(-1, model_width), expert_gate[0], expert_up[0])
    expert_out = lax.psum_scatter(
        jnp.dot(hidden, expert_down[0], preferred_element_type=jnp.float32).astype(jnp.bfloat16),
        "tp",
        scatter_dimension=0,
        tiled=True,
    )
    returned = lax.all_to_all(
        expert_out.reshape(sp_size, capacity, model_width),
        "sp",
        split_axis=0,
        concat_axis=0,
        tiled=True,
    )
    picked = jnp.take(returned.reshape(-1, model_width), own_pos, axis=0)
    picked = picked.reshape(rows_dev, top_count, model_width)
    own_weights = lax.dynamic_slice_in_dim(route_weights, own_begin, rows_dev, 0)
    routed = jnp.sum(picked.astype(jnp.float32) * own_weights[:, :, None], axis=1)
    hidden = gated(normed, shared_gate, shared_up)
    shared = lax.psum_scatter(
        jnp.dot(hidden, shared_down, preferred_element_type=jnp.float32).astype(jnp.bfloat16),
        "tp",
        scatter_dimension=0,
        tiled=True,
    ).astype(jnp.float32)
    own_resid = lax.dynamic_slice_in_dim(residual, own_begin, rows_dev, 0).astype(jnp.float32)
    return (own_resid + routed + shared).astype(jnp.bfloat16)


def brought(pairs, sems):
    copies = [
        pltpu.make_async_copy(source, target, sems.at[place])
        for place, (source, target) in enumerate(pairs)
    ]
    for copy in copies:
        copy.start()
    return copies


def pool_kernel(
    rim_ref, pooled_hbm, weight_hbm, scale_hbm, *refs
):
    pieces, (mixed_ref, pooled_ref, weight_ref, scale_ref, sems) = refs[:-5], refs[-5:]
    rows = pieces[0].shape[0] // 2
    tp_index = lax.axis_index("tp")
    copies = brought(
        ((pooled_hbm, pooled_ref), (weight_hbm, weight_ref), (scale_hbm, scale_ref)), sems
    )
    for copy in copies:
        copy.wait()
    tok_dev = pooled_ref.shape[0]
    window = lax.shift_left(jnp.int32(2), lax.axis_index("tp"))
    channels = pooled_ref[...].astype(jnp.float32)
    summed = jnp.concatenate([rim_ref[...].astype(jnp.float32), channels], 0)
    chosen, reach = summed, 1
    while reach < REACH:
        summed = summed + pltpu.roll(summed, reach, 0)
        reach *= 2
        chosen = jnp.where(window == reach, summed, chosen)
    position = lax.axis_index("sp") * tok_dev + lax.broadcasted_iota(jnp.int32, (tok_dev, 1), 0)
    counted = jnp.minimum(position + 1, window).astype(jnp.float32)
    pooled = (chosen[REACH:] / counted - channels).astype(jnp.bfloat16)
    mixed = jnp.dot(pooled, weight_ref[0], preferred_element_type=jnp.float32)
    mixed_ref[...] = (mixed * scale_ref[...]).astype(jnp.bfloat16)
    for flip, piece in enumerate(pieces):
        for place, block in enumerate((tp_index ^ flip, tp_index ^ flip ^ X_BIT)):
            begin = pl.multiple_of(block * rows, rows)
            piece[place * rows : (place + 1) * rows] = mixed_ref[pl.ds(begin, rows)]


def norm_kernel(*refs):
    groups, refs = refs[:-15], refs[-15:]
    routes_hbm, route_weights_hbm, stream_hbm, weight_hbm, gain_hbm = refs[:5]
    packed_ref, resid_ref, wide_ref, stream_ref, weight_ref, gain_ref, table_ref = refs[5:12]
    routes_ref, route_weights_ref, sems = refs[12:]
    rows, width = resid_ref.shape
    parts, depth, _ = weight_ref.shape
    tp_index = lax.axis_index("tp")
    places = [pl.multiple_of(block * rows, rows) for block in (tp_index, tp_index ^ X_BIT)]
    pairs = []
    for part in range(parts):
        begin = pl.multiple_of((tp_index ^ part) * depth, depth)
        pairs.append((weight_hbm.at[pl.ds(begin, depth)], weight_ref.at[part]))
    for place, begin in enumerate(places):
        pairs.append((stream_hbm.at[pl.ds(begin, rows)], stream_ref.at[pl.ds(place * rows, rows)]))
    pairs.append((gain_hbm, gain_ref))
    pairs = [(routes_hbm, routes_ref), (route_weights_hbm, route_weights_ref)] + pairs
    first, second, *copies = brought(pairs, sems)
    first.wait()
    second.wait()

    experts = lax.axis_size("sp")
    named = routes_ref[...]
    share = route_weights_ref[...]
    shape = (table_ref.shape[1], named.shape[1])
    line = lax.broadcasted_iota(jnp.int32, shape, 0)
    table = jnp.zeros(shape, jnp.float32)
    for choice in range(named.shape[0]):
        asked = named[choice : choice + 1]
        hit = (line == asked) | (line == asked + experts)
        table = table + jnp.where(hit, share[choice : choice + 1], 0.0)
    high = table.astype(jnp.bfloat16).astype(jnp.float32)
    table = jnp.where(line < experts, high, table - high)
    table_ref[...] = jnp.transpose(table).astype(jnp.bfloat16)
    for place, begin in enumerate(places):
        packed_ref[place * rows : (place + 1) * rows, width:] = table_ref[pl.ds(begin, rows)]

    block = min(512, width)
    blocks = [slice(start, start + block) for start in range(0, width, block)]
    for part, group in enumerate(groups):
        copies[part].wait()
        for cols in blocks:
            mixed = jnp.dot(
                group[...], weight_ref[part, :, cols], preferred_element_type=jnp.float32
            )
            wide_ref[:, cols] = mixed if part == 0 else wide_ref[:, cols] + mixed
    for copy in copies[parts:]:
        copy.wait()
    squares = jnp.zeros((2 * rows, 1), jnp.float32)
    for cols in blocks:
        residual = (stream_ref[:, cols].astype(jnp.float32) + wide_ref[:, cols]).astype(
            jnp.bfloat16
        )
        resid_ref[:, cols] = residual[:rows]
        wide = residual.astype(jnp.float32)
        wide_ref[:, cols] = wide
        squares = squares + jnp.sum(wide * wide, axis=1, keepdims=True)
    factor = lax.rsqrt(squares / width + EPSILON)
    for cols in blocks:
        packed_ref[:, cols] = (wide_ref[:, cols] * factor * gain_ref[:, cols]).astype(jnp.bfloat16)


def expert_kernel(n_pieces, takes, n_outs, with_shared, *refs):
    pieces = refs[:n_pieces]
    weights = refs[n_pieces : n_pieces + (12 if with_shared else 6)]
    outs = refs[n_pieces + len(weights) :][:n_outs]
    rows_ref, scale_ref, hidden_ref, shared_ref = refs[-4:]
    width = outs[0].shape[1]
    experts = lax.axis_size("sp")
    mine = lax.axis_index("sp")
    begin = 0
    for place, first, count in takes:
        taken = slice(first, first + count)
        rows_ref[begin : begin + count] = pieces[place][taken, :width]
        marks = pieces[place][taken, width:].astype(jnp.float32)
        lane = lax.broadcasted_iota(jnp.int32, marks.shape, 1)
        named = (lane == mine) | (lane == mine + experts)
        scale_ref[begin : begin + count] = jnp.sum(
            jnp.where(named, marks, 0.0), axis=1, keepdims=True
        )
        begin += count

    def fill(target, gates, ups, block):
        column = 0
        for gate, up in zip(gates, ups):
            for start in range(0, gate.shape[1], block):
                cols = slice(start, start + block)
                a = jnp.dot(rows_ref[...], gate[:, cols], preferred_element_type=jnp.float32)
                b = jnp.dot(rows_ref[...], up[:, cols], preferred_element_type=jnp.float32)
                target[:, column : column + block] = (jax.nn.silu(a) * b).astype(jnp.bfloat16)
                column += block

    def product(source, downs, cols):
        total, column = None, 0
        for down in downs:
            depth = down.shape[0]
            part = jnp.dot(
                source[:, column : column + depth], down[:, cols],
                preferred_element_type=jnp.float32,
            )
            total = part if total is None else total + part
            column += depth
        return total

    fill(hidden_ref, weights[0:2], weights[2:4], 256)
    if with_shared:
        fill(shared_ref, weights[6:8], weights[8:10], 128)
    share = begin // n_outs
    block = min(512, width)
    for start in range(0, width, block):
        cols = slice(start, start + block)
        value = product(hidden_ref, weights[4:6], cols) * scale_ref[...]
        if with_shared:
            value = value + product(shared_ref, weights[10:12], cols)
        value = value.astype(jnp.bfloat16)
        for place, out in enumerate(outs):
            out[:, cols] = value[place * share : (place + 1) * share]


def pass_kernel(source, target):
    target[...] = source[...]


def passing(token):
    return pl.pallas_call(
        pass_kernel,
        out_shape=jax.ShapeDtypeStruct(token.shape, token.dtype),
        in_specs=in_vmem(1),
        out_specs=in_vmem(1)[0],
        compiler_params=pltpu.CompilerParams(vmem_limit_bytes=MIB),
    )(token)


def in_vmem(count):
    return [pl.BlockSpec(memory_space=pltpu.VMEM)] * count


def kept_in_hbm(*arrays):
    return [pltpu.with_memory_space_constraint(array, pltpu.HBM) for array in arrays]


def in_hbm(count):
    return [pl.BlockSpec(memory_space=pltpu.HBM)] * count


def run_expert(pieces, weights, n_outs, width, takes=None):
    takes = takes or [(place, 0, piece.shape[0]) for place, piece in enumerate(pieces)]
    count = sum(take[2] for take in takes)
    with_shared = len(weights) == 12
    hidden = weights[0].shape[1] * 2
    shared = weights[6].shape[1] * 2 if with_shared else 128
    out = jax.ShapeDtypeStruct((count // n_outs, width), jnp.bfloat16)
    return pl.pallas_call(
        functools.partial(expert_kernel, len(pieces), tuple(takes), n_outs, with_shared),
        out_shape=[out] * n_outs,
        in_specs=in_vmem(len(pieces) + len(weights)),
        out_specs=in_vmem(n_outs),
        scratch_shapes=[
            pltpu.VMEM((count, width), jnp.bfloat16),
            pltpu.VMEM((count, 1), jnp.float32),
            pltpu.VMEM((count, hidden), jnp.bfloat16),
            pltpu.VMEM((count, shared), jnp.bfloat16),
        ],
        compiler_params=pltpu.CompilerParams(vmem_limit_bytes=16 * MIB),
    )(*pieces, *weights)


def tied(*values):
    return lax.optimization_barrier(values)


def dense_plan(
    stream, pooled_in, pool_weight, pool_scale, out_weight, norm_gain, routes, route_weights,
    expert_gate, expert_up, expert_down, shared_gate, shared_up, shared_down,
):
    tok_dev, width = stream.shape
    tp_size = lax.axis_size("tp")
    sp_size = lax.axis_size("sp")
    rows = tok_dev // tp_size
    f32, bf16 = jnp.float32, jnp.bfloat16
    y_bit = tp_size
    z_bits = [2 * tp_size * k for k in range(sp_size // 2)]

    rim_rows = passed_along(pooled_in[tok_dev - REACH :], "sp", 1)
    weights = []
    for weight in (expert_gate[0], expert_up[0], expert_down[0]):
        weights += [weight, swapped(weight, CORE_BIT)]
    shared_weights = []
    for weight in (shared_gate, shared_up, shared_down):
        shared_weights += [weight, swapped(weight, CORE_BIT)]

    lanes = -(-2 * sp_size // 128) * 128
    piece = jax.ShapeDtypeStruct((2 * rows, pooled_in.shape[1]), bf16)
    pool = pl.pallas_call(
        pool_kernel,
        out_shape=[piece] * tp_size,
        in_specs=in_vmem(1) + in_hbm(3),
        out_specs=in_vmem(tp_size),
        scratch_shapes=[
            pltpu.VMEM(pooled_in.shape, bf16),
            pltpu.VMEM(pooled_in.shape, bf16),
            pltpu.VMEM(pool_weight.shape, bf16),
            pltpu.VMEM((1, pool_scale.size), f32),
            pltpu.SemaphoreType.DMA((3,)),
        ],
        compiler_params=pltpu.CompilerParams(vmem_limit_bytes=4 * MIB),
    )
    groups = pool(rim_rows, *kept_in_hbm(pooled_in, pool_weight, pool_scale[None]))
    groups = [swapped(group, flip) if flip else group for flip, group in enumerate(groups)]
    depth = out_weight.shape[0] // tp_size
    norm = pl.pallas_call(
        norm_kernel,
        out_shape=[
            jax.ShapeDtypeStruct((2 * rows, width + lanes), bf16),
            jax.ShapeDtypeStruct((rows, width), bf16),
        ],
        in_specs=in_vmem(tp_size) + in_hbm(5),
        out_specs=in_vmem(2),
        scratch_shapes=[
            pltpu.VMEM((2 * rows, width), f32),
            pltpu.VMEM((2 * rows, width), bf16),
            pltpu.VMEM((tp_size, depth, width), bf16),
            pltpu.VMEM((1, width), f32),
            pltpu.VMEM((tok_dev, lanes), bf16),
            pltpu.VMEM(routes.shape[::-1], jnp.int32),
            pltpu.VMEM(routes.shape[::-1], f32),
            pltpu.SemaphoreType.DMA((tp_size + 5,)),
        ],
        compiler_params=pltpu.CompilerParams(vmem_limit_bytes=10 * MIB),
    )
    pair, own_resid = norm(
        *groups,
        *kept_in_hbm(routes.T, route_weights.T, stream, out_weight, norm_gain[None]),
    )

    kept, sent, got = {}, {}, {}
    z_1, z_2, _ = z_bits[1:]
    far_2 = swapped(pair[:rows], z_2)
    near = swapped(pair, y_bit)
    (kept[0],) = run_expert([pair], weights + shared_weights, 1, width)
    far_2, kept[0] = tied(far_2, kept[0])
    far_3 = swapped(far_2, z_1)
    y_2 = swapped(far_2, y_bit)
    x_2 = swapped(far_2, X_BIT)
    near, far_2 = tied(near, far_2)
    pair, far_2 = tied(pair, far_2)
    next_z = swapped(pair, z_1)
    other_z = swapped(near, z_1)
    (sent[0],) = run_expert([near], weights, 1, width)
    y_2, sent[0] = tied(y_2, sent[0])
    xy_2 = swapped(y_2, X_BIT)
    far_3, y_2 = tied(far_3, y_2)
    y_3 = swapped(far_3, y_bit)
    x_3 = swapped(far_3, X_BIT)
    token = passing(jnp.zeros((8, 128), f32))
    y_3, far_3 = tied(y_3, far_3)
    xy_3 = swapped(y_3, X_BIT)
    sent[0], y_3 = tied(sent[0], y_3)
    got[0] = swapped(sent[0], y_bit)
    xy_2, y_3 = tied(xy_2, y_3)
    blocks = [(place, 0, rows) for place in range(4)]
    kept[2], sent[2] = run_expert([far_2, y_2, x_2, xy_2, token], weights, 2, width, blocks)
    got[2] = swapped(sent[2], X_BIT)
    token = passing(token)
    xy_3, sent[2] = tied(xy_3, sent[2])
    kept[3], sent[3] = run_expert([far_3, x_3, y_3, xy_3, token], weights, 2, width, blocks)
    got[3] = swapped(sent[3], y_bit)
    next_z, sent[3] = tied(next_z, sent[3])
    takes = [(0, 0, rows), (1, 0, rows), (0, rows, rows), (1, rows, rows)]
    kept[1], sent[1] = run_expert([next_z, other_z], weights, 2, width, takes)
    got[1] = swapped(sent[1], X_BIT)

    def half(k, which):
        part = slice(which * rows, (which + 1) * rows)
        return kept[k][part].astype(f32) + got[k][part].astype(f32)

    def passed_on(k):
        flip = y_bit if k in (1, 2) else X_BIT
        return swapped(half(k, 1).astype(bf16), flip)

    def finished(k):
        flow = (half(k, 0) + more[k].astype(f32)).astype(bf16)
        return swapped(flow, z_bits[k])

    more, flows = {}, {}
    got[2], sent[1] = tied(got[2], sent[1])
    more[2] = passed_on(2)
    more[0] = passed_on(0)
    got[3], got[2] = tied(got[3], got[2])
    more[3] = passed_on(3)
    more[2], got[3] = tied(more[2], got[3])
    flows[2] = finished(2)
    wide = passing(own_resid.astype(f32))
    base = passing(half(0, 0) + wide)
    more[1] = passed_on(1)
    flows[3] = finished(3)
    flows[1] = finished(1)
    result = base + more[0].astype(f32)
    for k in (2, 3, 1):
        result = result + flows[k].astype(f32)
    return result.astype(bf16)


def on_device(
    stream,
    pooled_in,
    pool_weight,
    pool_scale,
    out_weight,
    norm_gain,
    routes,
    route_weights,
    *experts,
):
    sp_size = lax.axis_size("sp")
    tp_size = lax.axis_size("tp")
    tok_dev = stream.shape[0]
    capacity = max(2, 2 * (tok_dev // tp_size) * routes.shape[1] // sp_size)
    crowded = 2 * sp_size * tp_size * capacity >= sp_size * tok_dev
    paired = tp_size == 4 and sp_size == 8
    pooling = (stream, pooled_in, pool_weight, pool_scale, out_weight, norm_gain)
    if crowded and paired:
        return dense_plan(*pooling, routes, route_weights, *experts)
    residual, normed = mixer(*pooling)
    return routed_plan(residual, normed, routes, route_weights, *experts)


def solution(mesh):
    placed = (
        P("sp", None),
        P("sp", "tp"),
        P("tp", None, None),
        P("tp"),
        P(),
        P(),
        P("sp", None),
        P("sp", None),
        P("sp", None, "tp"),
        P("sp", None, "tp"),
        P("sp", "tp", None),
        P(None, "tp"),
        P(None, "tp"),
        P("tp", None),
    )
    return jax.shard_map(
        on_device, mesh=mesh, in_specs=placed, out_specs=P(("sp", "tp"), None), check_vma=False
    )
```
